512 devices in a mesh: sp: 64 (over z, y), tp: 8 (over x, core).
Axes of the slice: x: 4, y: 4, z: 16, core: 2. Of those that a mesh axis runs over, the one named last changes fastest.
Arguments:
- tokens: bfloat16 [32768, 2048], P('sp', 'tp'), may hold values from -6 to 6
- norm_gain: float32 [2048], replicated, may hold values from 0.1 to 1.9
- outer_gate: bfloat16 [2048, 1024], P('sp', 'tp'), may hold values from -0.125 to 0.125
- inner_gate: bfloat16 [2048, 1024], P('sp', 'tp'), may hold values from -0.125 to 0.125
- conv_input: bfloat16 [2048, 1024], P('sp', 'tp'), may hold values from -0.125 to 0.125
- query_proj: bfloat16 [2048, 1024], P('sp', 'tp'), may hold values from -0.125 to 0.125
- key_proj: bfloat16 [2048, 1024], P('sp', 'tp'), may hold values from -0.125 to 0.125
- value_proj: bfloat16 [2048, 1024], P('sp', 'tp'), may hold values from -0.125 to 0.125
- out_gate: bfloat16 [2048, 1024], P('sp', 'tp'), may hold values from -0.125 to 0.125
- conv_taps: float32 [3, 1024], P(None, 'tp'), may hold values from -3.5 to 3.5
- log_decay: float32 [2, 16, 32768], P(None, 'tp', 'sp'), may hold values from -1.2 to 0, as said below
- head_gain: float32 [1024], P('tp'), may hold values from 0.1 to 1.9
- conv_output: bfloat16 [1024, 2048], P('tp', 'sp'), may hold values from -0.1875 to 0.1875
- retention_output: bfloat16 [1024, 2048], P('tp', 'sp'), may hold values from -0.1875 to 0.1875
Outputs:
- mixed: bfloat16 [32768, 2048], P(('sp', 'tp'))
The draws below stay inside these ranges and needn't reach their ends.
Inputs may be any that keep to these rules, and one draw needn't show every extreme that they name: `log_decay`: logarithms of per-position decays, below zero.
All inputs are finite; a program needn't handle non-finite values.
Results may differ from the reference program's by a relative error of at most 0.02.
Values may be sent and summed in bfloat16 or wider, within the bound.
A program may use at most 128 MiB of HBM per device.

```python
import math
import jax
import jax.numpy as jnp
from jax import lax

D = 2048
CONV_CH = 1024
HEAD_NUMBER = 16
HEAD_DIM = 64
TOK_DEV = 512
TOKEN_NUMBER = 32768
N_SP = 64
N_TP = 8


def draw_log_decay(key, part):
    key_sequence = jax.random.split(jax.random.fold_in(key, 17), 6)
    span_count = TOKEN_NUMBER // TOK_DEV
    is_fast = jax.random.uniform(key_sequence[0], (2, HEAD_NUMBER, 1), jnp.float32) < 0.5
    fast_rate = jax.random.uniform(key_sequence[1], (2, HEAD_NUMBER, 1), jnp.float32, 0.01, 0.02)
    slow_rate = jax.random.uniform(key_sequence[2], (2, HEAD_NUMBER, 1), jnp.float32, 0.1, 0.3) / TOKEN_NUMBER
    selected_rate = jnp.where(is_fast, fast_rate, slow_rate)
    multiplier = jnp.exp(jax.random.uniform(key_sequence[3], (2, HEAD_NUMBER, span_count), jnp.float32, 0.0, math.log(4.0)))
    multiplier = jnp.repeat(multiplier, TOK_DEV, axis=2)
    flurry_location = jax.random.randint(key_sequence[4], (2, HEAD_NUMBER, 2, 1), 0, TOKEN_NUMBER)
    flurry_depth = jax.random.uniform(key_sequence[5], (2, HEAD_NUMBER, 2, 1), jnp.float32, 0.22, 0.51)
    position_list = jnp.arange(TOKEN_NUMBER, dtype=jnp.int32)
    flurry_list = jnp.sum(jnp.where(position_list == flurry_location, flurry_depth, 0.0), axis=2)
    return (-(selected_rate * multiplier) - flurry_list).astype(jnp.float32)


def shard_levels(stream_key, dims, pieces, least, largest):
    gain, own = 1.0, jax.random.fold_in(stream_key, 6)
    for axis_at, blocks in pieces:
        steps = jnp.exp(jax.random.uniform(jax.random.fold_in(own, axis_at), (blocks,), jnp.float32, least / len(pieces), largest / len(pieces)))
        gain = gain * jnp.repeat(steps, dims[axis_at] // blocks).reshape([-1 if axis == axis_at else 1 for axis in range(len(dims))])
    return gain


def centred(stream_key, dims, width, reach, cuts=(), held_as=jnp.bfloat16):
    gain = shard_levels(stream_key, dims, cuts, -0.22, 0.18) if cuts else 1.0
    entries = jax.random.normal(stream_key, dims, jnp.float32) * width * gain
    return jnp.minimum(jnp.maximum(entries, -reach), reach).astype(held_as)


def setup_inputs(seed: int = 0) -> dict:
    seeds = jax.random.split(jax.random.key(seed), 15)
    tokens = centred(seeds[0], (TOKEN_NUMBER, D), 1.0, 6.0, ((0, 64), (1, 8)))
    norm_gain = jnp.clip(1.0 + 0.18 * jax.random.normal(seeds[1], (D,), jnp.float32), 0.1, 1.9)
    outer_gate = centred(seeds[2], (D, CONV_CH), D ** -0.5, 0.125, ((0, 64), (1, 8)))
    inner_gate = centred(seeds[3], (D, CONV_CH), D ** -0.5, 0.125, ((0, 64), (1, 8)))
    conv_input = centred(seeds[4], (D, CONV_CH), D ** -0.5, 0.125, ((0, 64), (1, 8)))
    query_proj = centred(seeds[5], (D, HEAD_NUMBER * HEAD_DIM), D ** -0.5, 0.125, ((0, 64), (1, 8)))
    key_proj = centred(seeds[6], (D, HEAD_NUMBER * HEAD_DIM), D ** -0.5, 0.125, ((0, 64), (1, 8)))
    value_proj = centred(seeds[7], (D, HEAD_NUMBER * HEAD_DIM), D ** -0.5, 0.125, ((0, 64), (1, 8)))
    out_gate = centred(seeds[8], (D, HEAD_NUMBER * HEAD_DIM), D ** -0.5, 0.125, ((0, 64), (1, 8)))
    conv_taps = centred(seeds[9], (3, CONV_CH), 3 ** -0.5, 3.5, ((1, 8),), jnp.float32)
    log_decay = draw_log_decay(jax.random.fold_in(seeds[14], 71), 0)
    head_gain = jnp.clip(1.0 + 0.18 * jax.random.normal(seeds[11], (HEAD_NUMBER * HEAD_DIM,), jnp.float32), 0.1, 1.9)
    conv_output = centred(seeds[12], (CONV_CH, D), CONV_CH ** -0.5, 0.1875, ((0, 8), (1, 64)))
    retention_output = centred(seeds[13], (HEAD_NUMBER * HEAD_DIM, D), (HEAD_NUMBER * HEAD_DIM) ** -0.5, 0.1875, ((0, 8), (1, 64)))
    return {"tokens": tokens, "norm_gain": norm_gain, "outer_gate": outer_gate, "inner_gate": inner_gate, "conv_input": conv_input, "query_proj": query_proj, "key_proj": key_proj, "value_proj": value_proj, "out_gate": out_gate, "conv_taps": conv_taps, "log_decay": log_decay, "head_gain": head_gain, "conv_output": conv_output, "retention_output": retention_output}


EPS = 1e-06
THETA = 10000.0

def rounded(array):
    return lax.optimization_barrier(array.astype(jnp.bfloat16)).astype(jnp.float32)

def rotate(field_in, position_list):
    half_dim = field_in.shape[-1] // 2
    frequency = jnp.exp(-jnp.log(THETA) * jnp.arange(half_dim, dtype=jnp.float32) * (2.0 / field_in.shape[-1]))
    angles = position_list.astype(jnp.float32)[:, None, None] * frequency
    cosine = jnp.cos(angles)
    sine_part = jnp.sin(angles)
    leading = field_in[..., :half_dim]
    trailing = field_in[..., half_dim:]
    return jnp.concatenate([leading * cosine - trailing * sine_part, leading * sine_part + trailing * cosine], axis=-1)

def span_parts(query_rows, key_rows, value_rows, log_rates):
    length = query_rows.shape[0]
    forward_cum = jnp.cumsum(log_rates[0], axis=-1)
    backward_cum = jnp.flip(jnp.cumsum(jnp.flip(log_rates[1], -1), axis=-1), -1)
    row_index = lax.broadcasted_iota(jnp.int32, (length, length), 0)
    col_index = lax.broadcasted_iota(jnp.int32, (length, length), 1)
    lower_part = (col_index <= row_index)[None]
    spread = jnp.where(lower_part, forward_cum[:, :, None] - forward_cum[:, None, :], backward_cum[:, :, None] - backward_cum[:, None, :])
    scores = jnp.einsum('ihe,jhe->hij', query_rows.astype(jnp.float32), key_rows.astype(jnp.float32))
    weighted = rounded(scores * jnp.exp(spread))
    local_part = jnp.einsum('hij,jhe->ihe', weighted, value_rows.astype(jnp.float32))
    key_wide = key_rows.astype(jnp.float32)
    forward_keys = rounded(key_wide * jnp.exp(forward_cum[:, -1:] - forward_cum).T[:, :, None])
    backward_keys = rounded(key_wide * jnp.exp(backward_cum[:, :1] - backward_cum).T[:, :, None])
    forward_state = jnp.einsum('jhd,jhe->hde', forward_keys, value_rows.astype(jnp.float32))
    backward_state = jnp.einsum('jhd,jhe->hde', backward_keys, value_rows.astype(jnp.float32))
    return (local_part, forward_cum, backward_cum, forward_state, backward_state)

def span_item(inputs):
    return span_parts(inputs[0], inputs[1], inputs[2], inputs[3])

def carried(query_rows, forward_cum, backward_cum, into_forward, into_backward):
    query_wide = query_rows.astype(jnp.float32)
    forward_part = jnp.einsum('ihd,hde->ihe', query_wide, rounded(into_forward))
    backward_part = jnp.einsum('ihd,hde->ihe', query_wide, rounded(into_backward))
    return jnp.exp(forward_cum).T[:, :, None] * forward_part + jnp.exp(backward_cum).T[:, :, None] * backward_part

def finish(mixed_heads, gate_rows, head_gain):
    row_count, head_count, head_width = mixed_heads.shape
    scaled = mixed_heads * lax.rsqrt(lax.optimization_barrier(jnp.mean(mixed_heads * mixed_heads, axis=-1, keepdims=True)) + EPS)
    scaled = scaled * head_gain.reshape(head_count, head_width)
    return (jax.nn.silu(gate_rows.astype(jnp.float32)) * scaled.reshape(row_count, head_count * head_width)).astype(jnp.bfloat16)

def forward_step(running, inputs):
    return (jnp.exp(inputs[0])[:, None, None] * running + inputs[1], running)

def reference(tokens, norm_gain, outer_gate, inner_gate, conv_input, query_proj, key_proj, value_proj, out_gate, conv_taps, log_decay, head_gain, conv_output, retention_output):
    wide = tokens.astype(jnp.float32)
    normed = (wide * lax.rsqrt(lax.optimization_barrier(jnp.mean(wide * wide, axis=-1, keepdims=True)) + EPS) * norm_gain).astype(jnp.bfloat16)
    projected = [jnp.dot(normed, weight, preferred_element_type=jnp.float32).astype(jnp.bfloat16) for weight in (outer_gate, inner_gate, conv_input, query_proj, key_proj, value_proj, out_gate)]
    inner_value = (projected[1].astype(jnp.float32) * projected[2].astype(jnp.float32)).astype(jnp.bfloat16)
    padded = jnp.pad(inner_value.astype(jnp.float32), ((1, 1), (0, 0)))
    convolved = conv_taps[0] * padded[:-2] + conv_taps[1] * padded[1:-1] + conv_taps[2] * padded[2:]
    conv_out = (projected[0].astype(jnp.float32) * convolved).astype(jnp.bfloat16)
    position_list = jnp.arange(TOKEN_NUMBER, dtype=jnp.int32)
    shape_heads = (TOKEN_NUMBER, HEAD_NUMBER, HEAD_DIM)
    rotated_query = rotate(projected[3].astype(jnp.float32).reshape(shape_heads), position_list).astype(jnp.bfloat16)
    rotated_key = (rotate(projected[4].astype(jnp.float32).reshape(shape_heads), position_list) * HEAD_DIM ** (-0.5)).astype(jnp.bfloat16)
    value_heads = projected[5].reshape(shape_heads)
    span_shape = (N_SP, TOK_DEV, HEAD_NUMBER, HEAD_DIM)
    span_rates = log_decay.reshape(2, HEAD_NUMBER, N_SP, TOK_DEV).transpose(2, 0, 1, 3)
    span_query = rotated_query.reshape(span_shape)
    local_part, forward_cum, backward_cum, forward_state, backward_state = lax.map(span_item, (span_query, rotated_key.reshape(span_shape), value_heads.reshape(span_shape), span_rates))
    blank = jnp.zeros((HEAD_NUMBER, HEAD_DIM, HEAD_DIM), jnp.float32)
    into_forward = lax.scan(forward_step, blank, (forward_cum[:, :, -1], forward_state))[1]
    into_backward = lax.scan(forward_step, blank, (backward_cum[:, :, 0], backward_state), reverse=True)[1]
    carried_part = jax.vmap(carried)(span_query, forward_cum, backward_cum, into_forward, into_backward)
    mixed_heads = (local_part + carried_part).reshape(shape_heads)
    ret_out = finish(mixed_heads, projected[6], head_gain)
    conv_group = CONV_CH // N_TP
    ret_group = HEAD_NUMBER * HEAD_DIM // N_TP
    total_sum = jnp.zeros((TOKEN_NUMBER, D), jnp.float32)
    for group_index in range(N_TP):
        conv_lo = group_index * conv_group
        ret_lo = group_index * ret_group
        partial_sum = jnp.dot(conv_out[:, conv_lo:conv_lo + conv_group], conv_output[conv_lo:conv_lo + conv_group], preferred_element_type=jnp.float32)
        partial_sum = partial_sum + jnp.dot(ret_out[:, ret_lo:ret_lo + ret_group], retention_output[ret_lo:ret_lo + ret_group], preferred_element_type=jnp.float32)
        total_sum = total_sum + rounded(partial_sum)
    return total_sum.astype(jnp.bfloat16)
```

```python
import functools
import jax
import jax.numpy as jnp
from jax import lax
from jax.sharding import PartitionSpec as P
from jax.experimental import pallas as pl
from jax.experimental.pallas import tpu as pltpu

NZ, NY, NX = 16, 4, 4
MESH = pl.DeviceIdType.MESH
BROWS, AROWS = 96, 192
BF = jnp.bfloat16
F32 = jnp.float32


def place():
    s, t = lax.axis_index("sp"), lax.axis_index("tp")
    z, y = s // NY, lax.rem(s, NY)
    x, c = t // 2, lax.rem(t, 2)
    return s, t, z, y, x, c


def ring(value, step, size):
    return lax.rem(value + (step + size), size)


def gather_kernel(tok, w, X, WA, WB, loc, zas, zar, zbs, zbr, yas, yar, ybs, ybr, xs, xr):
    s, t, z, y, x, c = place()

    def at(dz=0, dy=0, dx=0, dc=0):
        return (ring(z, dz, NZ) * NY + ring(y, dy, NY), ring(x, dx, NX) * 2 + ring(c, dc, 2))

    own = [
        pltpu.make_async_copy(w.at[pl.ds(BROWS, AROWS)], WA.at[z, y], loc.at[0]),
        pltpu.make_async_copy(w.at[pl.ds(0, BROWS)], WB.at[z, y], loc.at[1]),
        pltpu.make_async_copy(tok.at[:, pl.ds(0, 128)], X.at[2 * t], loc.at[2]),
        pltpu.make_async_copy(tok.at[:, pl.ds(128, 128)], X.at[2 * t + 1], loc.at[3]),
    ]
    for o in own:
        o.start()
    barrier = pltpu.get_barrier_semaphore()
    near = [at(dz=1), at(dz=-1), at(dy=1), at(dy=-1), at(dx=1), at(dx=-1), at(dc=1)]
    for d in near:
        pl.semaphore_signal(barrier, inc=1, device_id=d, device_id_type=MESH)
    for o in own:
        o.wait()
    pl.semaphore_wait(barrier, len(near))

    sent = []

    def push(ref, ssem, rsem, dev):
        cp = pltpu.make_async_remote_copy(src_ref=ref, dst_ref=ref, send_sem=ssem, recv_sem=rsem, device_id=dev, device_id_type=MESH)
        cp.start()
        sent.append(cp)

    def took(ref, ssem, rsem):
        pltpu.make_async_remote_copy(src_ref=ref, dst_ref=ref, send_sem=ssem, recv_sem=rsem, device_id=at(dz=1), device_id_type=MESH).wait_recv()

    DZ = (1, -1)

    def za(k, d):
        return (pl.ds(0, AROWS) if k < 8 else pl.ds(d * (AROWS // 2), AROWS // 2))

    def zb(k, d):
        return (pl.ds(0, BROWS) if k < 8 else pl.ds(d * (BROWS // 2), BROWS // 2))

    def send_za(k):
        for d in (0, 1):
            o = ring(z, -DZ[d] * (k - 1), NZ)
            push(WA.at[o, y, za(k, d)], zas.at[d, k - 1], zar.at[d, k - 1], at(dz=DZ[d]))

    def recv_za(k):
        for d in (0, 1):
            o = ring(z, -DZ[d] * k, NZ)
            took(WA.at[o, y, za(k, d)], zas.at[d, k - 1], zar.at[d, k - 1])

    def send_zb(k, j):
        for d in (0, 1):
            o = ring(z, -DZ[d] * (k - 1), NZ)
            push(WB.at[o, ring(y, j, NY), zb(k, d)], zbs.at[d, k - 1, j], zbr.at[d, k - 1, j], at(dz=DZ[d]))

    def recv_zb(k, j):
        for d in (0, 1):
            o = ring(z, -DZ[d] * k, NZ)
            took(WB.at[o, ring(y, j, NY), zb(k, d)], zbs.at[d, k - 1, j], zbr.at[d, k - 1, j])

    def y_direct(buf, o, ss, rr):
        for d in (0, 1):
            push(buf.at[o, y], ss(d), rr(d), at(dy=DZ[d]))

    def y_onward(buf, o, ss, rr, rows):
        for d in (0, 1):
            src = ring(y, -DZ[d], NY)
            took(buf.at[o, src], ss(d), rr(d))
            push(buf.at[o, src, pl.ds(d * (rows // 2), rows // 2)], ss(2 + d), rr(2 + d), at(dy=DZ[d]))

    def y_last(buf, o, ss, rr, rows):
        for d in (0, 1):
            src = ring(y, -2 * DZ[d], NY)
            took(buf.at[o, src, pl.ds(d * (rows // 2), rows // 2)], ss(2 + d), rr(2 + d))

    def sem2(ref, i):
        return lambda d: ref.at[d, i]

    def ya(i):
        return sem2(yas, i), sem2(yar, i)

    def origins(k):
        if k == 0:
            return [(0, z)]
        if k == 8:
            return [(15, ring(z, 8, NZ))]
        return [(k, ring(z, -k, NZ)), (7 + k, ring(z, k, NZ))]

    def xblk(tt, half=None):
        base = 2 * tt
        return X.at[pl.ds(base, 2)] if half is None else X.at[base + half]

    def same(dx):
        return ring(x, dx, NX) * 2 + c

    for d in (0, 1):
        push(xblk(t), xs.at[d], xr.at[d], at(dx=DZ[d]))
    ybf = lambda d: ybs.at[d]
    ybg = lambda d: ybr.at[d]
    y_direct(WB, z, ybf, ybg)
    send_zb(1, 0)
    send_za(1)
    y_direct(WA, z, *ya(0))
    push(xblk(t), xs.at[4], xr.at[4], at(dc=1))
    y_onward(WB, z, ybf, ybg, BROWS)
    send_zb(1, 1)
    send_zb(1, 3)
    y_last(WB, z, ybf, ybg, BROWS)
    send_zb(1, 2)
    for k in range(1, 9):
        recv_za(k)
        if k < 8:
            send_za(k + 1)
        for i, o in origins(k):
            y_direct(WA, o, *ya(i))
        for j in (0, 1, 3, 2):
            recv_zb(k, j)
            if k < 8:
                send_zb(k + 1, j)
        for i, o in origins(k - 1):
            y_onward(WA, o, *ya(i), AROWS)
        if k == 2:
            for d in (0, 1):
                took(xblk(same(-DZ[d])), xs.at[d], xr.at[d])
                push(xblk(same(-DZ[d]), d), xs.at[2 + d], xr.at[2 + d], at(dx=DZ[d]))
                push(xblk(same(-DZ[d])), xs.at[5 + d], xr.at[5 + d], at(dc=1))
        if k == 4:
            for d in (0, 1):
                took(xblk(same(-2 * DZ[d]), d), xs.at[2 + d], xr.at[2 + d])
            push(xblk(same(2)), xs.at[7], xr.at[7], at(dc=1))
        if k == 5:
            took(xblk(ring(t, 0, 8) + 1 - 2 * c), xs.at[4], xr.at[4])
            for d in (0, 1):
                took(xblk(ring(x, -DZ[d], NX) * 2 + 1 - c), xs.at[5 + d], xr.at[5 + d])
            took(xblk(ring(x, 2, NX) * 2 + 1 - c), xs.at[7], xr.at[7])
    for i, o in origins(8):
        y_onward(WA, o, *ya(i), AROWS)
    for i in range(16):
        pass
    for k in range(0, 9):
        for i, o in origins(k):
            y_last(WA, o, *ya(i), AROWS)
    for cp in sent:
        cp.wait_send()


def gather(tok, w):
    D = pltpu.SemaphoreType.DMA
    vm = pl.BlockSpec(memory_space=pltpu.VMEM)
    anys = pl.BlockSpec(memory_space=pl.ANY)
    return pl.pallas_call(
        gather_kernel,
        out_shape=[
            jax.ShapeDtypeStruct((16, 512, 128), BF),
            jax.ShapeDtypeStruct((NZ, NY, AROWS, 128), BF),
            jax.ShapeDtypeStruct((NZ, NY, BROWS, 128), BF),
        ],
        in_specs=[anys, anys],
        out_specs=[vm] * 3,
        scratch_shapes=[
            D((4,)), D((2, 8)), D((2, 8)), D((2, 8, 4)), D((2, 8, 4)),
            D((4, 16)), D((4, 16)), D((4,)), D((4,)), D((8,)), D((8,)),
        ],
        compiler_params=pltpu.CompilerParams(collective_id=0, has_side_effects=True, vmem_limit_bytes=48 * 1024 * 1024),
    )(tok, w)

HEAD_DIM = 64


EPS = 1e-06
THETA = 10000.0


def with_halo(shard, sides, width):
    for axis, dim in sides:
        size, length = (lax.axis_size(axis), shard.shape[dim])
        up = [(i, (i + 1) % size) for i in range(size - 1)]
        down = [(j, i) for i, j in up]
        last = lax.slice_in_dim(shard, length - width, length, axis=dim)
        first = lax.slice_in_dim(shard, 0, width, axis=dim)
        before = lax.ppermute(last, axis, up)
        after = lax.ppermute(first, axis, down)
        shard = jnp.concatenate([before, shard, after], axis=dim)
    return shard


def from_everyone(shard, axis):
    copies = jnp.broadcast_to(shard, (lax.axis_size(axis), *shard.shape))
    return lax.all_to_all(copies, axis, split_axis=0, concat_axis=0, tiled=True)


def in_order(parts, dim):
    shape = list(parts.shape[1:])
    shape[dim] *= parts.shape[0]
    return jnp.moveaxis(parts, 0, dim).reshape(shape)


def collect(shard, axis, dim):
    parts = from_everyone(shard, axis)
    return in_order(parts, dim)


def in_one_piece(arrays, axis, dim, along):
    ends, at = ([], 0)
    for a in arrays[:-1]:
        at += a.shape[along]
        ends.append(at)
    both = jnp.concatenate(arrays, axis=along)
    return tuple(jnp.split(lax.all_gather(both, axis, axis=dim, tiled=True), ends, axis=along))


def turned_gather(arrays, axis, dims):
    turned = [jnp.moveaxis(a, dim, 0) for a, dim in zip(arrays, dims)]
    both = jnp.concatenate([t.reshape(len(t), -1) for t in turned], axis=1)
    filled, at, finished = (lax.all_gather(both, axis, axis=0, tiled=True), 0, [])
    for t, dim in zip(turned, dims):
        piece = filled[:, at : at + t[0].size].reshape(-1, *t.shape[1:])
        finished.append(jnp.moveaxis(piece, 0, dim))
        at += t[0].size
    return tuple(finished)


def in_blocks(shard, dim, size):
    before, after = (shard.shape[:dim], shard.shape[dim + 1 :])
    return jnp.moveaxis(shard.reshape(*before, size, -1, *after), dim, 0)


def sum_at_owner(shard, axis, dim):
    parts = in_blocks(shard, dim, lax.axis_size(axis))
    arrived = lax.all_to_all(parts, axis, split_axis=0, concat_axis=0, tiled=True)
    return arrived.astype(jnp.float32).sum(axis=0)


def rotate(field_in, position_list):
    half_dim = field_in.shape[-1] // 2
    frequency = jnp.exp(
        -jnp.log(THETA) * jnp.arange(half_dim, dtype=jnp.float32) * (2.0 / field_in.shape[-1])
    )
    angles = position_list.astype(jnp.float32)[:, None, None] * frequency
    cosine = jnp.cos(angles)
    sine_part = jnp.sin(angles)
    leading = field_in[..., :half_dim]
    trailing = field_in[..., half_dim:]
    return jnp.concatenate(
        [leading * cosine - trailing * sine_part, leading * sine_part + trailing * cosine], axis=-1
    )


def conv_branch(outer_rows, inner_rows, conv_values, conv_taps):
    inner_value = (inner_rows.astype(jnp.float32) * conv_values.astype(jnp.float32)).astype(
        jnp.bfloat16
    )
    padded = with_halo(inner_value, (("sp", 0),), 1).astype(jnp.float32)
    convolved = conv_taps[0] * padded[:-2] + conv_taps[1] * padded[1:-1] + conv_taps[2] * padded[2:]
    return (outer_rows.astype(jnp.float32) * convolved).astype(jnp.bfloat16)


def span_parts(query_rows, key_rows, value_rows, log_rates):
    length = query_rows.shape[0]
    forward_cum = jnp.cumsum(log_rates[0], axis=-1)
    backward_cum = jnp.flip(jnp.cumsum(jnp.flip(log_rates[1], -1), axis=-1), -1)
    row_index = lax.broadcasted_iota(jnp.int32, (length, length), 0)
    col_index = lax.broadcasted_iota(jnp.int32, (length, length), 1)
    lower_part = (col_index <= row_index)[None]
    spread = jnp.where(
        lower_part,
        forward_cum[:, :, None] - forward_cum[:, None, :],
        backward_cum[:, :, None] - backward_cum[:, None, :],
    )
    scores = jnp.einsum("ihe,jhe->hij", query_rows, key_rows, preferred_element_type=jnp.float32)
    weighted = (scores * jnp.exp(spread)).astype(jnp.bfloat16)
    local_part = jnp.einsum(
        "hij,jhe->ihe", weighted, value_rows, preferred_element_type=jnp.float32
    )
    key_wide = key_rows.astype(jnp.float32)
    forward_keys = (key_wide * jnp.exp(forward_cum[:, -1:] - forward_cum).T[:, :, None]).astype(
        jnp.bfloat16
    )
    backward_keys = (key_wide * jnp.exp(backward_cum[:, :1] - backward_cum).T[:, :, None]).astype(
        jnp.bfloat16
    )
    forward_state = jnp.einsum(
        "jhd,jhe->hde", forward_keys, value_rows, preferred_element_type=jnp.float32
    )
    backward_state = jnp.einsum(
        "jhd,jhe->hde", backward_keys, value_rows, preferred_element_type=jnp.float32
    )
    return (local_part, forward_cum, backward_cum, forward_state, backward_state)


def retention_branch(query_rows, key_rows, value_rows, gate_rows, log_decay, head_gain, offsets):
    row_count = query_rows.shape[0]
    head_count = query_rows.shape[1] // HEAD_DIM
    shape_heads = (row_count, head_count, HEAD_DIM)
    rotated_query = rotate(query_rows.astype(jnp.float32).reshape(shape_heads), offsets).astype(
        jnp.bfloat16
    )
    rotated_key = (
        rotate(key_rows.astype(jnp.float32).reshape(shape_heads), offsets) * HEAD_DIM ** (-0.5)
    ).astype(jnp.bfloat16)
    local_part, forward_cum, backward_cum, forward_state, backward_state = span_parts(
        rotated_query, rotated_key, value_rows.reshape(shape_heads), log_decay
    )
    forward_total = forward_cum[:, -1]
    backward_total = backward_cum[:, 0]
    totals = collect(jnp.stack([forward_total, backward_total])[None], "sp", 0)
    inclusive = jnp.cumsum(totals, axis=0)
    exclusive = inclusive - totals
    own_index = lax.axis_index("sp")
    own_inclusive = lax.dynamic_index_in_dim(inclusive, own_index, 0, keepdims=False)
    own_exclusive = lax.dynamic_index_in_dim(exclusive, own_index, 0, keepdims=False)
    pieces = in_one_piece((forward_state[None], backward_state[None]), "sp", 0, 1)
    piece_count = pieces[0].shape[0]
    span_index = lax.iota(jnp.int32, piece_count)
    forward_weight = jnp.where(
        (span_index < own_index)[:, None],
        jnp.exp(jnp.minimum(own_exclusive[0] - inclusive[:, 0], 0.0)),
        0.0,
    )
    backward_weight = jnp.where(
        (span_index > own_index)[:, None],
        jnp.exp(jnp.minimum(exclusive[:, 1] - own_inclusive[1], 0.0)),
        0.0,
    )
    into_forward = jnp.einsum("nh,nhde->hde", forward_weight, pieces[0])
    into_backward = jnp.einsum("nh,nhde->hde", backward_weight, pieces[1])
    forward_part = jnp.einsum(
        "ihd,hde->ihe",
        rotated_query,
        into_forward.astype(jnp.bfloat16),
        preferred_element_type=jnp.float32,
    )
    backward_part = jnp.einsum(
        "ihd,hde->ihe",
        rotated_query,
        into_backward.astype(jnp.bfloat16),
        preferred_element_type=jnp.float32,
    )
    mixed_heads = (
        local_part
        + jnp.exp(forward_cum).T[:, :, None] * forward_part
        + jnp.exp(backward_cum).T[:, :, None] * backward_part
    )
    scaled = mixed_heads * lax.rsqrt(
        jnp.mean(mixed_heads * mixed_heads, axis=-1, keepdims=True) + EPS
    )
    scaled = scaled * head_gain.reshape(head_count, HEAD_DIM)
    return (
        jax.nn.silu(gate_rows.astype(jnp.float32))
        * scaled.reshape(row_count, head_count * HEAD_DIM)
    ).astype(jnp.bfloat16)


def local(
    tokens,
    norm_gain,
    outer_gate,
    inner_gate,
    conv_input,
    query_proj,
    key_proj,
    value_proj,
    out_gate,
    conv_taps,
    log_decay,
    head_gain,
    conv_output,
    retention_output,
):
    order = (key_proj, value_proj, query_proj, out_gate, inner_gate, conv_input, outer_gate, conv_output.T, retention_output.T)
    blocks, wa, wb = gather(tokens, jnp.concatenate(order, axis=0))
    whole = jnp.moveaxis(blocks, 0, 1).reshape(512, 2048)
    wa = wa.reshape(64, 6, 32, 128)
    wb = wb.reshape(64, 3, 32, 128)
    pick = lambda a, i: a[:, i].reshape(2048, 128)
    wide = whole.astype(jnp.float32)
    normed = (
        wide * lax.rsqrt(jnp.mean(wide * wide, axis=-1, keepdims=True) + EPS) * norm_gain
    ).astype(jnp.bfloat16)
    row_count = normed.shape[0]
    offsets = lax.axis_index("sp") * row_count + lax.iota(jnp.int32, row_count)
    gathered = [pick(wa, 3), pick(wa, 1), pick(wa, 2), pick(wb, 2), pick(wb, 0), pick(wb, 1), pick(wa, 0), pick(wa, 4).T, pick(wa, 5).T]
    projected = [
        jnp.dot(normed, weight, preferred_element_type=jnp.float32).astype(jnp.bfloat16)
        for weight in gathered[:7]
    ]
    conv_out = conv_branch(projected[0], projected[1], projected[2], conv_taps)
    ret_out = retention_branch(
        projected[3], projected[4], projected[5], projected[6], log_decay, head_gain, offsets
    )
    conv_weight = gathered[7]
    ret_weight = gathered[8]
    mixed = sum_at_owner(
        (
            jnp.dot(conv_out, conv_weight, preferred_element_type=jnp.float32)
            + jnp.dot(ret_out, ret_weight, preferred_element_type=jnp.float32)
        ).astype(jnp.bfloat16),
        "tp",
        0,
    )
    return mixed.astype(jnp.bfloat16)


def solution(mesh):
    return jax.shard_map(
        local,
        mesh=mesh,
        in_specs=(
            P("sp", "tp"),
            P(),
            P("sp", "tp"),
            P("sp", "tp"),
            P("sp", "tp"),
            P("sp", "tp"),
            P("sp", "tp"),
            P("sp", "tp"),
            P("sp", "tp"),
            P(None, "tp"),
            P(None, "tp", "sp"),
            P("tp"),
            P("tp", "sp"),
            P("tp", "sp"),
        ),
        out_specs=P(("sp", "tp"), None),
        check_vma=False,
    )
```

```python
import math

import jax
import jax.numpy as jnp
from jax import lax
from jax.experimental import pallas as pl
from jax.experimental.pallas import tpu as pltpu
from jax.sharding import PartitionSpec as P

NZ, NY, NX = 16, 4, 4
SPAN, HEAD = 512, 64
EPS, THETA = 1e-06, 10000.0
BROWS, AROWS = 96, 192
MESH = pl.DeviceIdType.MESH
BF, F32 = jnp.bfloat16, jnp.float32
EXACT = lax.Precision.HIGHEST
SIDES = (1, -1)


def ring(value, step, size):
    return lax.rem(value + (step + size), size)


def rows_of(i, n):
    return pl.ds(pl.multiple_of(i * n, n), n)


def nn(a, b, precision=None):
    return lax.dot_general(a, b, (((1,), (0,)), ((), ())), precision=precision, preferred_element_type=F32)


def nt(a, b, precision=None):
    return lax.dot_general(a, b, (((1,), (1,)), ((), ())), precision=precision, preferred_element_type=F32)


def tn(a, b):
    return lax.dot_general(a, b, (((0,), (0,)), ((), ())), preferred_element_type=F32)


def left_head(shape):
    return lax.broadcasted_iota(jnp.int32, shape, len(shape) - 1) < HEAD


def mixer_kernel(
    tok, gain, outer_w, inner_w, conv_w, query_w, key_w, value_w, gate_w, taps, decay, head_gain, conv_o, ret_o,
    out,
    X, NR, WA, WB, WO, accb, acca, D, scale, trig, qkv, mix, CR, halo_s, halo_r,
    msg_a, got_a, msg_b, got_b, msg_c, got_c, part, pair, quads, via, fin,
    loc, zas, zar, zbs, zbr, yas, yar, ybs, ybr, xs, xr, hs, hr, sas, sar, sbs, sbr, scs, scr, ds, dr, vs, vr, fs, fr,
):
    s, t = lax.axis_index("sp"), lax.axis_index("tp")
    z, y, x, c = s // NY, lax.rem(s, NY), t // 2, lax.rem(t, 2)

    def at(dz=0, dy=0, dx=0, dc=0):
        return (ring(z, dz, NZ) * NY + ring(y, dy, NY), ring(x, dx, NX) * 2 + ring(c, dc, 2))

    sent = []

    def push(src, dst, ssem, rsem, dev):
        cp = pltpu.make_async_remote_copy(
            src_ref=src, dst_ref=dst, send_sem=ssem, recv_sem=rsem, device_id=dev, device_id_type=MESH
        )
        cp.start()
        sent.append(cp)

    def took(ref, ssem, rsem):
        pltpu.make_async_remote_copy(
            src_ref=ref, dst_ref=ref, send_sem=ssem, recv_sem=rsem, device_id=at(dz=1), device_id_type=MESH
        ).wait_recv()

    own = [
        pltpu.make_async_copy(tok.at[:, pl.ds(0, 128)], X.at[2 * t], loc.at[0]),
        pltpu.make_async_copy(tok.at[:, pl.ds(128, 128)], X.at[2 * t + 1], loc.at[1]),
    ]
    for i, w in enumerate((key_w, value_w, query_w)):
        own.append(pltpu.make_async_copy(w, WB.at[z, y, pl.ds(32 * i, 32)], loc.at[2 + i]))
    for i, w in enumerate((gate_w, inner_w, conv_w, outer_w)):
        own.append(pltpu.make_async_copy(w, WA.at[z, y, pl.ds(32 * i, 32)], loc.at[5 + i]))
    for o in own:
        o.start()
    WA[z, y, pl.ds(128, 32)] = conv_o[...]
    WA[z, y, pl.ds(160, 32)] = ret_o[...]
    barrier = pltpu.get_barrier_semaphore()
    near = [at(dz=1), at(dz=-1), at(dy=1), at(dy=-1), at(dx=1), at(dx=-1), at(dc=1)]
    for d in near:
        pl.semaphore_signal(barrier, inc=1, device_id=d, device_id_type=MESH)
    for o in own:
        o.wait()
    pl.semaphore_wait(barrier, len(near))

    def half_or_all(k, d, rows):
        return pl.ds(0, rows) if k < 8 else pl.ds(d * (rows // 2), rows // 2)

    def send_za(k):
        for d in (0, 1):
            ref = WA.at[ring(z, -SIDES[d] * (k - 1), NZ), y, half_or_all(k, d, AROWS)]
            push(ref, ref, zas.at[d, k - 1], zar.at[d, k - 1], at(dz=SIDES[d]))

    def recv_za(k):
        for d in (0, 1):
            took(WA.at[ring(z, -SIDES[d] * k, NZ), y, half_or_all(k, d, AROWS)], zas.at[d, k - 1], zar.at[d, k - 1])

    def send_zb(k, j):
        for d in (0, 1):
            ref = WB.at[ring(z, -SIDES[d] * (k - 1), NZ), ring(y, j, NY), half_or_all(k, d, BROWS)]
            push(ref, ref, zbs.at[d, k - 1, j], zbr.at[d, k - 1, j], at(dz=SIDES[d]))

    def recv_zb(k, j):
        for d in (0, 1):
            ref = WB.at[ring(z, -SIDES[d] * k, NZ), ring(y, j, NY), half_or_all(k, d, BROWS)]
            took(ref, zbs.at[d, k - 1, j], zbr.at[d, k - 1, j])

    def y_direct(buf, o, ss, rr):
        for d in (0, 1):
            push(buf.at[o, y], buf.at[o, y], ss(d), rr(d), at(dy=SIDES[d]))

    def y_onward(buf, o, ss, rr, rows):
        for d in (0, 1):
            src = ring(y, -SIDES[d], NY)
            took(buf.at[o, src], ss(d), rr(d))
            ref = buf.at[o, src, pl.ds(d * (rows // 2), rows // 2)]
            push(ref, ref, ss(2 + d), rr(2 + d), at(dy=SIDES[d]))

    def y_last(buf, o, ss, rr, rows):
        for d in (0, 1):
            src = ring(y, -2 * SIDES[d], NY)
            took(buf.at[o, src, pl.ds(d * (rows // 2), rows // 2)], ss(2 + d), rr(2 + d))

    def ya(i):
        return (lambda d: yas.at[d, i]), (lambda d: yar.at[d, i])

    def origins(k):
        if k == 0:
            return [(0, z)]
        if k == 8:
            return [(15, ring(z, 8, NZ))]
        return [(k, ring(z, -k, NZ)), (7 + k, ring(z, k, NZ))]

    yb = (lambda d: ybs.at[d]), (lambda d: ybr.at[d])

    def xblk(tt, half=None):
        return X.at[pl.ds(2 * tt, 2)] if half is None else X.at[2 * tt + half]

    def on_x(dx, core):
        return ring(x, dx, NX) * 2 + core

    def xpush(tt, half, i, dev):
        push(xblk(tt, half), xblk(tt, half), xs.at[i], xr.at[i], dev)

    def decay_sums():
        row = lax.broadcasted_iota(jnp.int32, (SPAN, SPAN), 0)
        col = lax.broadcasted_iota(jnp.int32, (SPAN, SPAN), 1)
        lower = (col <= row).astype(F32)
        upper = (col >= row).astype(F32)
        for i, tri in enumerate((lower, upper)):
            rates = decay[i]
            along = jnp.concatenate([rates, jnp.zeros((6, SPAN), F32)], axis=0)
            over = nt(along, tri, EXACT)
            mix[pl.ds(i * 8, 8), :] = over
            columns = [nt(tri, jnp.broadcast_to(rates[h : h + 1], (128, SPAN)), EXACT) for h in (0, 1)]
            for h in (0, 1):
                scale[2 * i + h] = columns[h]

    def decay_matrix(h):
        row = lax.broadcasted_iota(jnp.int32, (128, SPAN), 0)
        col = lax.broadcasted_iota(jnp.int32, (128, SPAN), 1)

        def chunk(i, _):
            wide = lambda a: jnp.concatenate([a] * 4, axis=1)
            cf = wide(scale[h, rows_of(i, 128)]) - mix[pl.ds(h, 1), :]
            rb = wide(scale[2 + h, rows_of(i, 128)]) - mix[pl.ds(8 + h, 1), :]
            D[h, rows_of(i, 128)] = jnp.exp(jnp.where(col <= row + i * 128, cf, rb))
            return 0

        lax.fori_loop(0, 4, chunk, 0)

    def decay_scales():
        left = left_head((SPAN, 128))
        cf = jnp.where(left, scale[0], scale[1])
        rb = jnp.where(left, scale[2], scale[3])
        scale[0] = jnp.exp(cf)
        scale[1] = jnp.exp(rb)
        scale[2] = jnp.exp(cf[SPAN - 1 : SPAN] - cf)
        scale[3] = jnp.exp(rb[0:1] - rb)
        tot = jnp.where(lax.broadcasted_iota(jnp.int32, (8, 128), 0) == 0, cf[SPAN - 1 : SPAN], rb[0:1])
        for q in range(NY):
            msg_a[q, pl.ds(32, 8)] = tot

    def angles():
        def chunk(i, _):
            lane = lax.broadcasted_iota(jnp.int32, (128, 128), 1)
            pos = (lax.broadcasted_iota(jnp.int32, (128, 128), 0) + (s * SPAN + i * 128)).astype(F32)
            freq = jnp.exp(-math.log(THETA) * lax.rem(lane, 32).astype(F32) * (2.0 / HEAD))
            ang = pos * freq
            trig[0, rows_of(i, 128)] = jnp.cos(ang)
            sine = jnp.sin(ang)
            trig[1, rows_of(i, 128)] = jnp.where(lax.rem(lane, HEAD) < HEAD // 2, -sine, sine)
            return 0

        lax.fori_loop(0, 4, chunk, 0)

    def normalise():
        def chunk(i, _):
            r = rows_of(i, 64)
            total = jnp.zeros((64, 128), F32)
            for b in range(16):
                w = X[b, r].astype(F32)
                total = total + w * w
            inv = lax.rsqrt(jnp.sum(total, axis=1, keepdims=True) * (1.0 / 2048) + EPS)
            for b in range(16):
                NR[b, r] = (X[b, r].astype(F32) * inv * gain[pl.ds(b, 1), :]).astype(BF)
            return 0

        lax.fori_loop(0, 8, chunk, 0)

    def project(buf, acc, count, k):
        o1, o2 = (ring(z, -k, NZ), ring(z, k, NZ)) if k else (z, ring(z, 8, NZ))
        lhs = jnp.concatenate([NR[o1], NR[o2]], axis=1)
        for i in range(count):
            w = jnp.concatenate([buf[o, :, pl.ds(32 * i, 32), :].reshape(128, 128) for o in (o1, o2)], axis=0)
            part_sum = nn(lhs, w)
            acc[i] = part_sum if k == 1 else acc[i] + part_sum

    def turn_output(k):
        for _, o in origins(k):
            for i in (0, 1):
                w = WA[o, :, pl.ds(128 + 32 * i, 32), :].reshape(128, 128)
                WO[pl.ds(128 * i, 128), pl.ds(pl.multiple_of(o * 128, 128), 128)] = w.T

    def rotated(a):
        wide = a.astype(BF).astype(F32)
        first = lax.rem(lax.broadcasted_iota(jnp.int32, wide.shape, 1), HEAD) < HEAD // 2
        other = jnp.where(first, pltpu.roll(wide, 96, axis=1), pltpu.roll(wide, 32, axis=1))
        return wide * trig[0] + other * trig[1]

    def states():
        rk = (rotated(accb[0]) * HEAD**-0.5).astype(BF)
        value = accb[1].astype(BF)
        qkv[1] = rk
        qkv[2] = value
        wide = rk.astype(F32)
        left = left_head((HEAD, 128))
        for i in (0, 1):
            full = tn((wide * scale[2 + i]).astype(BF), value)
            packed = jnp.where(left, full[0:HEAD], full[HEAD:])
            for q in range(NY):
                msg_a[q, pl.ds(16 * i, 16)] = packed[16 * q : 16 * q + 16]

    def attend():
        qkv[0] = rotated(accb[2]).astype(BF)
        rk, value = qkv[1], qkv[2]

        def chunk(i, _):
            r = rows_of(i, 128)
            rq = qkv[0, r]
            left = left_head((128, 128))
            zero = jnp.zeros_like(rq)
            parts = []
            for h, own_q in enumerate((jnp.where(left, rq, zero), jnp.where(left, zero, rq))):
                probs = (nt(own_q, rk) * D[h, r]).astype(BF)
                parts.append(nn(probs, value))
            mix[r, pl.ds(0, 128)] = jnp.where(left, parts[0], parts[1])
            return 0

        lax.fori_loop(0, 4, chunk, 0)

    def inner_value():
        return (acca[1].astype(BF).astype(F32) * acca[2].astype(BF).astype(F32)).astype(BF).astype(F32)

    def halo_send():
        inner = inner_value()
        halo_s[0] = inner[0:8]
        halo_s[1] = inner[SPAN - 8 :]
        push(halo_s.at[1], halo_r.at[0], hs.at[0], hr.at[0], (lax.rem(s + 1, NZ * NY), t))
        push(halo_s.at[0], halo_r.at[1], hs.at[1], hr.at[1], (lax.rem(s + NZ * NY - 1, NZ * NY), t))

    def convolve():
        for i in (0, 1):
            took(halo_r.at[i], hs.at[i], hr.at[i])
        inner = inner_value()
        row = lax.broadcasted_iota(jnp.int32, (SPAN, 128), 0)
        before = jnp.where(s == 0, 0.0, halo_r[0, 7:8, :])
        after = jnp.where(s == NZ * NY - 1, 0.0, halo_r[1, 0:1, :])
        prev = jnp.where(row == 0, before, pltpu.roll(inner, 1, axis=0))
        follow = jnp.where(row == SPAN - 1, after, pltpu.roll(inner, SPAN - 1, axis=0))
        conv = taps[0:1, :] * prev + taps[1:2, :] * inner + taps[2:3, :] * follow
        CR[:, pl.ds(0, 128)] = (acca[3].astype(BF).astype(F32) * conv).astype(BF)

    def spread_states():
        for dy in (1, 2, 3):
            yy = ring(y, dy, NY)
            push(msg_a.at[yy], got_a.at[y], sas.at[dy - 1], sar.at[dy - 1], at(dy=dy))
        got_a[y] = msg_a[y]

    def step_terms():
        return [
            (got_a[m, pl.ds(0, 16)], got_a[m, pl.ds(16, 16)], jnp.exp(got_a[m, pl.ds(32, 1)]), jnp.exp(got_a[m, pl.ds(33, 1)]))
            for m in range(NY)
        ]

    def spread_rows():
        for dy in (1, 2, 3):
            took(got_a.at[ring(y, -dy, NY)], sas.at[dy - 1], sar.at[dy - 1])
        terms = step_terms()
        fwd, bwd = terms[0][0], terms[NY - 1][1]
        for m in range(1, NY):
            fwd = terms[m][2] * fwd + terms[m][0]
            back = terms[NY - 1 - m]
            bwd = back[3] * bwd + back[1]
        msg_b[0, pl.ds(0, 16)] = fwd
        msg_b[1, pl.ds(0, 16)] = bwd
        for i in (0, 1):
            total = got_a[0, pl.ds(32 + i, 1)]
            for m in range(1, NY):
                total = total + got_a[m, pl.ds(32 + i, 1)]
            msg_b[i, pl.ds(16, 8)] = jnp.broadcast_to(total, (8, 128))
        for d in (8, 7, 9, 6, 10, 5, 11, 4, 12, 3, 13, 2, 14, 1, 15):
            push(msg_b.at[(z + d) // NZ], got_b.at[d], sbs.at[d], sbr.at[d], at(dz=d))

    def return_rows():
        for d in range(1, NZ):
            took(got_b.at[d], sbs.at[d], sbr.at[d])
        fwd = jnp.zeros((16, 128), F32)
        bwd = jnp.zeros((16, 128), F32)
        for d in range(NZ - 1, 0, -1):
            lower = jnp.exp(got_b[d, pl.ds(16, 1)]) * fwd + got_b[d, pl.ds(0, 16)]
            fwd = jnp.where(d <= z, lower, fwd)
            e = NZ - d
            higher = jnp.exp(got_b[e, pl.ds(16, 1)]) * bwd + got_b[e, pl.ds(0, 16)]
            bwd = jnp.where(d <= NZ - 1 - z, higher, bwd)
        terms = step_terms()
        for m in range(NY):
            msg_c[m, pl.ds(0, 16)] = fwd.astype(BF)
            fwd = terms[m][2] * fwd + terms[m][0]
            n = NY - 1 - m
            msg_c[n, pl.ds(16, 16)] = bwd.astype(BF)
            bwd = terms[n][3] * bwd + terms[n][1]
        for dy in (2, 1, 3):
            yy = ring(y, dy, NY)
            push(msg_c.at[yy], got_c.at[y], scs.at[dy - 1], scr.at[dy - 1], at(dy=dy))
        got_c[y] = msg_c[y]

    def finish():
        for dy in (1, 2, 3):
            took(got_c.at[ring(y, -dy, NY)], scs.at[dy - 1], scr.at[dy - 1])
        left = left_head((HEAD, 128))
        into = []
        for i in (0, 1):
            packed = jnp.concatenate([got_c[q, pl.ds(16 * i, 16)] for q in range(NY)], axis=0)
            zero = jnp.zeros_like(packed)
            into.append(jnp.concatenate([jnp.where(left, packed, zero), jnp.where(left, zero, packed)], axis=0))
        both = jnp.concatenate(into, axis=1)
        same = (
            (lax.broadcasted_iota(jnp.int32, (128, 128), 0) < HEAD) == (lax.broadcasted_iota(jnp.int32, (128, 128), 1) < HEAD)
        ).astype(F32) * (1.0 / HEAD)

        def chunk(i, _):
            r = rows_of(i, 128)
            carried = nn(qkv[0, r], both)
            m = mix[r, pl.ds(0, 128)] + scale[0, r] * carried[:, :128] + scale[1, r] * carried[:, 128:]
            inv = lax.rsqrt(nn(m * m, same, EXACT) + EPS)
            g = acca[0, r].astype(BF).astype(F32)
            silu = g / (1.0 + jnp.exp(-g))
            CR[r, pl.ds(128, 128)] = (silu * (m * inv * head_gain[...])).astype(BF)
            return 0

        lax.fori_loop(0, 4, chunk, 0)

    def out_rows(xo):
        rows = CR[rows_of(ring(x, xo, NX), 128)]
        for n in range(4):
            cols = pl.ds(512 * n, 512)
            res = nn(rows, WO[:, cols]).astype(BF).reshape(2, 64, 512)
            part[xo, :, n // 2, :, pl.ds(512 * (n % 2), 512)] = res
        push(part.at[xo, 1 - c], pair.at[xo], ds.at[xo], dr.at[xo], at(dc=1))

    def summed(xo, half):
        return part[xo, c, half].astype(F32) + pair[xo, half].astype(F32)

    def reduce_out():
        for xo in (2, 1, 3, 0):
            out_rows(xo)
        took(pair.at[2], ds.at[2], dr.at[2])
        for h in (0, 1):
            quads[2, h] = summed(2, h).astype(BF)
            push(quads.at[2, h], via.at[h], vs.at[h], vr.at[h], at(dx=SIDES[h]))
        for xo, d in ((1, 0), (3, 1)):
            took(pair.at[xo], ds.at[xo], dr.at[xo])
            quads[xo, 1 - d] = summed(xo, 1 - d).astype(BF)
            push(quads.at[xo, 1 - d], fin.at[d, 1 - d], fs.at[d, 1 - d], fr.at[d, 1 - d], at(dx=SIDES[d]))
        for xo, d in ((1, 0), (3, 1)):
            took(via.at[d], vs.at[d], vr.at[d])
            quads[xo, d] = (summed(xo, d) + via[d].astype(F32)).astype(BF)
            push(quads.at[xo, d], fin.at[d, d], fs.at[d, d], fr.at[d, d], at(dx=SIDES[d]))
        took(pair.at[0], ds.at[0], dr.at[0])
        for h in (0, 1):
            for d in (0, 1):
                took(fin.at[d, h], fs.at[d, h], fr.at[d, h])
            out[:, pl.ds(1024 * h, 1024)] = (summed(0, h) + fin[0, h].astype(F32) + fin[1, h].astype(F32)).astype(BF)

    for d in (0, 1):
        xpush(t, None, d, at(dx=SIDES[d]))
    y_direct(WB, z, *yb)
    send_zb(1, 0)
    send_za(1)
    y_direct(WA, z, *ya(0))
    xpush(t, None, 4, at(dc=1))
    y_onward(WB, z, *yb, BROWS)
    send_zb(1, 1)
    send_zb(1, 3)
    y_last(WB, z, *yb, BROWS)
    send_zb(1, 2)
    decay_sums()
    for k in range(1, 9):
        recv_za(k)
        if k < 8:
            send_za(k + 1)
        for i, o in origins(k):
            y_direct(WA, o, *ya(i))
        for j in (0, 1, 3, 2):
            recv_zb(k, j)
            if k < 8:
                send_zb(k + 1, j)
        for i, o in origins(k - 1):
            y_onward(WA, o, *ya(i), AROWS)
        if k == 1:
            decay_matrix(0)
        if k == 2:
            for d in (0, 1):
                src = on_x(-SIDES[d], c)
                took(xblk(src), xs.at[d], xr.at[d])
                xpush(src, d, 2 + d, at(dx=SIDES[d]))
                xpush(src, None, 5 + d, at(dc=1))
            decay_matrix(1)
        if k == 3:
            decay_scales()
        if k == 4:
            for d in (0, 1):
                took(xblk(on_x(2, c), d), xs.at[2 + d], xr.at[2 + d])
            xpush(on_x(2, c), None, 7, at(dc=1))
            angles()
        if k == 5:
            took(xblk(on_x(0, 1 - c)), xs.at[4], xr.at[4])
            for d in (0, 1):
                took(xblk(on_x(-SIDES[d], 1 - c)), xs.at[5 + d], xr.at[5 + d])
            took(xblk(on_x(2, 1 - c)), xs.at[7], xr.at[7])
            normalise()
            project(WB, accb, 3, 1)
        if k == 6:
            for j in (2, 3, 4, 5):
                project(WB, accb, 3, j)
        if k == 7:
            for j in (6, 7):
                project(WB, accb, 3, j)
    for i, o in origins(8):
        y_onward(WA, o, *ya(i), AROWS)
    project(WB, accb, 3, 0)
    states()
    spread_states()
    for k in range(0, 9):
        for i, o in origins(k):
            y_last(WA, o, *ya(i), AROWS)
    for k in (1, 2, 3, 4, 5, 6, 7, 0):
        project(WA, acca, 4, k)
    halo_send()
    spread_rows()
    for k in range(9):
        turn_output(k)
    attend()
    convolve()
    return_rows()
    finish()
    reduce_out()
    for cp in sent:
        cp.wait_send()


def mixer(tok, gain, outer, inner, conv, query, key, value, gate, taps, decay, head_gain, conv_o, ret_o):
    dma = pltpu.SemaphoreType.DMA
    vm, anywhere = pl.BlockSpec(memory_space=pltpu.VMEM), pl.BlockSpec(memory_space=pl.ANY)
    return pl.pallas_call(
        mixer_kernel,
        out_shape=jax.ShapeDtypeStruct((64, 2048), BF),
        in_specs=[anywhere, vm] + [anywhere] * 7 + [vm] * 5,
        out_specs=vm,
        scratch_shapes=[
            pltpu.VMEM((16, SPAN, 128), BF),
            pltpu.VMEM((16, SPAN, 128), BF),
            pltpu.VMEM((NZ, NY, AROWS, 128), BF),
            pltpu.VMEM((NZ, NY, BROWS, 128), BF),
            pltpu.VMEM((256, 2048), BF),
            pltpu.VMEM((3, SPAN, 128), F32),
            pltpu.VMEM((4, SPAN, 128), F32),
            pltpu.VMEM((2, SPAN, SPAN), F32),
            pltpu.VMEM((4, SPAN, 128), F32),
            pltpu.VMEM((2, SPAN, 128), F32),
            pltpu.VMEM((3, SPAN, 128), BF),
            pltpu.VMEM((SPAN, 512), F32),
            pltpu.VMEM((SPAN, 256), BF),
            pltpu.VMEM((2, 8, 128), F32),
            pltpu.VMEM((2, 8, 128), F32),
            pltpu.VMEM((NY, 40, 128), F32),
            pltpu.VMEM((NY, 40, 128), F32),
            pltpu.VMEM((2, 24, 128), F32),
            pltpu.VMEM((NZ, 24, 128), F32),
            pltpu.VMEM((NY, 32, 128), BF),
            pltpu.VMEM((NY, 32, 128), BF),
            pltpu.VMEM((NX, 2, 2, 64, 1024), BF),
            pltpu.VMEM((NX, 2, 64, 1024), BF),
            pltpu.VMEM((NX, 2, 64, 1024), BF),
            pltpu.VMEM((2, 64, 1024), BF),
            pltpu.VMEM((2, 2, 64, 1024), BF),
            dma((9,)),
            dma((2, 8)), dma((2, 8)), dma((2, 8, 4)), dma((2, 8, 4)),
            dma((4, 16)), dma((4, 16)), dma((4,)), dma((4,)), dma((8,)), dma((8,)),
            dma((2,)), dma((2,)), dma((3,)), dma((3,)), dma((16,)), dma((16,)), dma((3,)), dma((3,)),
            dma((4,)), dma((4,)), dma((2,)), dma((2,)), dma((2, 2)), dma((2, 2)),
        ],
        compiler_params=pltpu.CompilerParams(
            collective_id=0, has_side_effects=True, vmem_limit_bytes=56 * 1024 * 1024
        ),
    )(
        tok, gain.reshape(16, 128), outer, inner, conv, query, key, value, gate, taps, decay,
        head_gain.reshape(1, 128), conv_o.T, ret_o.T,
    )


def solution(mesh):
    return jax.shard_map(
        mixer,
        mesh=mesh,
        in_specs=(
            P("sp", "tp"),
            P(),
            P("sp", "tp"),
            P("sp", "tp"),
            P("sp", "tp"),
            P("sp", "tp"),
            P("sp", "tp"),
            P("sp", "tp"),
            P("sp", "tp"),
            P(None, "tp"),
            P(None, "tp", "sp"),
            P("tp"),
            P("tp", "sp"),
            P("tp", "sp"),
        ),
        out_specs=P(("sp", "tp"), None),
        check_vma=False,
    )
```

```python
import math

import jax
import jax.numpy as jnp
from jax import lax
from jax.experimental import pallas as pl
from jax.experimental.pallas import tpu as pltpu
from jax.sharding import PartitionSpec as P

NZ, NY, NX = 16, 4, 4
SPAN, HEAD = 512, 64
EPS, THETA = 1e-06, 10000.0
KROWS, BROWS, AROWS = 64, 96, 128
MESH = pl.DeviceIdType.MESH
BF, F32 = jnp.bfloat16, jnp.float32
SIDES = (1, -1)


def ring(value, step, size):
    return lax.rem(value + (step + size), size)


def rows_of(i, n):
    return pl.ds(pl.multiple_of(i * n, n), n)


def nn(a, b):
    return lax.dot_general(a, b, (((1,), (0,)), ((), ())), preferred_element_type=F32)


def nt(a, b):
    return lax.dot_general(a, b, (((1,), (1,)), ((), ())), preferred_element_type=F32)


def tn(a, b):
    return lax.dot_general(a, b, (((0,), (0,)), ((), ())), preferred_element_type=F32)


def left_head(shape):
    return lax.broadcasted_iota(jnp.int32, shape, len(shape) - 1) < HEAD


def mixer_kernel(
    tok, gain_in, outer_w, inner_w, conv_w, query_w, key_w, value_w, gate_w, taps_in, decay_in, head_gain_in, conv_o, ret_o,
    out,
    gain, taps, decay, head_gain, X, NR, WK, WA, WB, WO, acck, accb, acca, D, scale, trig, qkv, mix, CR, halo_s, halo_r,
    msg_a, got_a, msg_b, got_b, msg_c, got_c, part, pair, quads, via, fin, done,
    loc, kzr, kyr, zar, zbr, yar, yahr, ybr, xr, hr, sar, sbr, scr, dr, vr, fr, ssem, outs,
):
    s, t = lax.axis_index("sp"), lax.axis_index("tp")
    z, y, x, c = s // NY, lax.rem(s, NY), t // 2, lax.rem(t, 2)

    def at(dz=0, dy=0, dx=0, dc=0):
        return (ring(z, dz, NZ) * NY + ring(y, dy, NY), ring(x, dx, NX) * 2 + ring(c, dc, 2))

    def push(src, dst, sem, rsem, dev):
        pltpu.make_async_remote_copy(
            src_ref=src, dst_ref=dst, send_sem=ssem.at[sem], recv_sem=rsem, device_id=dev, device_id_type=MESH
        ).start()

    def all_left(ref, sem):
        pltpu.make_async_remote_copy(
            src_ref=ref, dst_ref=ref, send_sem=ssem.at[sem], recv_sem=kyr.at[0], device_id=at(dz=1), device_id_type=MESH
        ).wait_send()

    def took(ref, rsem):
        pltpu.make_async_remote_copy(
            src_ref=ref, dst_ref=ref, send_sem=ssem.at[0], recv_sem=rsem, device_id=at(dz=1), device_id_type=MESH
        ).wait_recv()

    barrier = pltpu.get_barrier_semaphore()
    near = [at(dz=1), at(dz=-1), at(dz=2), at(dz=-2), at(dy=1), at(dy=-1), at(dy=2), at(dx=1), at(dx=-1), at(dc=1)]
    for d in near:
        pl.semaphore_signal(barrier, inc=1, device_id=d, device_id_type=MESH)
    moves = [(w, WK.at[z, y, pl.ds(32 * i, 32)]) for i, w in enumerate((key_w, value_w))]
    moves += [(w, WB.at[z, y, pl.ds(32 * i, 32)]) for i, w in enumerate((query_w, inner_w, conv_w))]
    moves += [(w, WA.at[z, y, pl.ds(32 * i, 32)]) for i, w in enumerate((gate_w, outer_w, conv_o, ret_o))]
    moves += [(tok.at[:, pl.ds(128 * i, 128)], X.at[2 * t + i]) for i in (0, 1)]
    moves += [(gain_in, gain), (taps_in, taps), (decay_in, decay), (head_gain_in, head_gain)]
    own = [pltpu.make_async_copy(a, b, loc.at[i]) for i, (a, b) in enumerate(moves)]
    for o in own:
        o.start()

    def own_here():
        for o in own:
            o.wait()

    def greeted():
        pl.semaphore_wait(barrier, len(near))

    def half_or_all(k, d, rows):
        return pl.ds(0, rows) if k < 8 else pl.ds(d * (rows // 2), rows // 2)

    def send_kv(k):
        for d in (0, 1):
            back = (k - 1) // 2 * 2
            ref = WK.at[ring(z, -SIDES[d] * back, NZ), y, half_or_all(k, d, KROWS)]
            push(ref, ref, 0, kzr.at[d, k - 1], at(dz=SIDES[d] * (k - back)))

    def recv_kv(k):
        for d in (0, 1):
            took(WK.at[ring(z, -SIDES[d] * k, NZ), y, half_or_all(k, d, KROWS)], kzr.at[d, k - 1])

    def y_kv(k):
        for _, o in origins(k):
            for dy in (2, 1, 3):
                push(WK.at[o, y], WK.at[o, y], 1, kyr.at[0], at(dy=dy))

    def send_za(k):
        for d in (0, 1):
            ref = WA.at[ring(z, -SIDES[d] * (k - 1), NZ), y, half_or_all(k, d, AROWS)]
            push(ref, ref, 2, zar.at[d, k - 1], at(dz=SIDES[d]))

    def recv_za(k):
        for d in (0, 1):
            took(WA.at[ring(z, -SIDES[d] * k, NZ), y, half_or_all(k, d, AROWS)], zar.at[d, k - 1])

    def send_zb(k, j):
        for d in (0, 1):
            ref = WB.at[ring(z, -SIDES[d] * (k - 1), NZ), ring(y, j, NY), half_or_all(k, d, BROWS)]
            push(ref, ref, 3, zbr.at[d, k - 1, j], at(dz=SIDES[d]))

    def recv_zb(k, j):
        for d in (0, 1):
            ref = WB.at[ring(z, -SIDES[d] * k, NZ), ring(y, j, NY), half_or_all(k, d, BROWS)]
            took(ref, zbr.at[d, k - 1, j])

    def side(d, rows):
        return pl.ds(d * (rows // 2), rows // 2)

    def ya_direct(k):
        for i, o in origins(k):
            for d in (0, 1):
                push(WA.at[o, y], WA.at[o, y], 4, yar.at[d, i], at(dy=SIDES[d]))

    def ya_onward(k):
        for i, o in origins(k):
            for d in (0, 1):
                src = ring(y, -SIDES[d], NY)
                took(WA.at[o, src], yar.at[d, i])
                ref = WA.at[o, src, side(d, AROWS)]
                push(ref, ref, 4, yahr.at[0 if k < 6 else 1], at(dy=SIDES[d]))

    def yb_direct():
        for dy in (2, 1, 3):
            push(WB.at[z, y], WB.at[z, y], 5, ybr.at[dy - 1], at(dy=dy))

    def yb_take(j):
        took(WB.at[z, ring(y, j, NY)], ybr.at[NY - 1 - j])

    def origins(k):
        if k == 0:
            return [(0, z)]
        if k == 8:
            return [(15, ring(z, 8, NZ))]
        return [(k, ring(z, -k, NZ)), (7 + k, ring(z, k, NZ))]

    def xblk(tt, half=None):
        return X.at[pl.ds(2 * tt, 2)] if half is None else X.at[2 * tt + half]

    def on_x(dx, core):
        return ring(x, dx, NX) * 2 + core

    def xpush(tt, half, i, dev):
        push(xblk(tt, half), xblk(tt, half), 6, xr.at[i], dev)

    def x_start():
        for d in (0, 1):
            for h in (d, 1 - d):
                xpush(t, h, 2 * d + h, at(dx=SIDES[d]))

    def x_onward():
        for d in (0, 1):
            src = on_x(-SIDES[d], c)
            took(xblk(src, d), xr.at[3 * d])
            xpush(src, d, 4 + d, at(dx=SIDES[d]))

    def x_partner():
        for d in (0, 1):
            src = on_x(-SIDES[d], c)
            took(xblk(src, 1 - d), xr.at[2 * d + 1 - d])
            xpush(src, None, 7 + d, at(dc=1))

    def x_far():
        for d in (0, 1):
            took(xblk(on_x(2, c), d), xr.at[4 + d])
        xpush(on_x(2, c), None, 9, at(dc=1))

    def x_all():
        took(xblk(on_x(0, 1 - c)), xr.at[6])
        for d in (0, 1):
            took(xblk(on_x(-SIDES[d], 1 - c)), xr.at[7 + d])
        took(xblk(on_x(2, 1 - c)), xr.at[9])

    def decay_sums():
        row = lax.broadcasted_iota(jnp.int32, (SPAN, SPAN), 0)
        col = lax.broadcasted_iota(jnp.int32, (SPAN, SPAN), 1)
        lower = jnp.where(col <= row, 1.0, 0.0).astype(BF)
        upper = jnp.where(col >= row, 1.0, 0.0).astype(BF)
        for i, (tri, turned) in enumerate(((lower, upper), (upper, lower))):
            rest = jnp.concatenate([jnp.broadcast_to(decay[i, h : h + 1, :], (128, SPAN)) for h in (0, 1)], axis=0)
            over, along = None, None
            for _ in range(3):
                term = rest.astype(BF)
                rest = rest - term.astype(F32)
                o, a = nt(tri, term), nn(jnp.concatenate([term[0:8], term[128:136]], axis=0), turned)
                over, along = (o, a) if over is None else (over + o, along + a)
            mix[pl.ds(16 * i, 16), :] = along
            for h in (0, 1):
                scale[2 * i + h] = over[:, 128 * h : 128 * h + 128]

    def decay_matrix(h):
        row = lax.broadcasted_iota(jnp.int32, (128, SPAN), 0)
        col = lax.broadcasted_iota(jnp.int32, (128, SPAN), 1)

        def chunk(i, _):
            wide = lambda a: jnp.concatenate([a] * 4, axis=1)
            cf = wide(scale[h, rows_of(i, 128)]) - mix[pl.ds(8 * h, 1), :]
            rb = wide(scale[2 + h, rows_of(i, 128)]) - mix[pl.ds(16 + 8 * h, 1), :]
            D[h, rows_of(i, 128)] = jnp.exp(jnp.where(col <= row + i * 128, cf, rb))
            return 0

        lax.fori_loop(0, 4, chunk, 0)

    def decay_scales():
        left = left_head((SPAN, 128))
        cf = jnp.where(left, scale[0], scale[1])
        rb = jnp.where(left, scale[2], scale[3])
        scale[0] = jnp.exp(cf)
        scale[1] = jnp.exp(rb)
        scale[2] = jnp.exp(cf[SPAN - 1 : SPAN] - cf)
        scale[3] = jnp.exp(rb[0:1] - rb)
        tot = jnp.where(lax.broadcasted_iota(jnp.int32, (8, 128), 0) == 0, cf[SPAN - 1 : SPAN], rb[0:1])
        for q in range(NY):
            msg_a[q, pl.ds(32, 8)] = tot

    def angles():
        def chunk(i, _):
            lane = lax.broadcasted_iota(jnp.int32, (128, 128), 1)
            pos = (lax.broadcasted_iota(jnp.int32, (128, 128), 0) + (s * SPAN + i * 128)).astype(F32)
            freq = jnp.exp(-math.log(THETA) * lax.rem(lane, 32).astype(F32) * (2.0 / HEAD))
            ang = pos * freq
            trig[0, rows_of(i, 128)] = jnp.cos(ang)
            sine = jnp.sin(ang)
            trig[1, rows_of(i, 128)] = jnp.where(lax.rem(lane, HEAD) < HEAD // 2, -sine, sine)
            return 0

        lax.fori_loop(0, 4, chunk, 0)

    def normalise():
        def chunk(i, _):
            r = rows_of(i, 64)
            total = jnp.zeros((64, 128), F32)
            for b in range(16):
                w = X[b, r].astype(F32)
                total = total + w * w
            inv = lax.rsqrt(jnp.sum(total, axis=1, keepdims=True) * (1.0 / 2048) + EPS)
            for b in range(16):
                NR[b, r] = (X[b, r].astype(F32) * inv * gain[pl.ds(b, 1), :]).astype(BF)
            return 0

        lax.fori_loop(0, 8, chunk, 0)

    def project_kv():
        def chunk(i, _):
            r = rows_of(i, 256)
            lhs = jnp.concatenate([NR[b, r] for b in range(NZ)], axis=1)
            w = [WK[:, :, pl.ds(32 * n, 32), :].reshape(2048, 128) for n in (0, 1)]
            both = nn(lhs, jnp.concatenate(w, axis=1))
            acck[0, r] = both[:, :128]
            acck[1, r] = both[:, 128:]
            return 0

        lax.fori_loop(0, 2, chunk, 0)

    def project_part(buf, acc, count, base, hops, first):
        os = [o for k in hops for _, o in origins(k)]
        lhs = jnp.concatenate([NR[o] for o in os], axis=1)
        for n in range(0, count):
            w = jnp.concatenate([buf[o, :, pl.ds(base + 32 * n, 32), :].reshape(128, 128) for o in os], axis=0)
            total = nn(lhs, w)
            acc[n] = total if first else acc[n] + total

    def project_b(*hops):
        project_part(WB, accb, 3, 0, hops, hops[0] == 1)

    def project_a(*hops):
        project_part(WA, acca, 2, 0, hops, hops[0] == 0)

    def turn_output(k):
        for _, o in origins(k):
            for i in (0, 1):
                w = WA[o, :, pl.ds(64 + 32 * i, 32), :].reshape(128, 128)
                WO[pl.ds(128 * i, 128), pl.ds(pl.multiple_of(o * 128, 128), 128)] = w.T

    def rotated(a):
        wide = a.astype(BF).astype(F32)
        first = lax.rem(lax.broadcasted_iota(jnp.int32, wide.shape, 1), HEAD) < HEAD // 2
        other = jnp.where(first, pltpu.roll(wide, 96, axis=1), pltpu.roll(wide, 32, axis=1))
        return wide * trig[0] + other * trig[1]

    def states():
        rk = (rotated(acck[0]) * HEAD**-0.5).astype(BF)
        value = acck[1].astype(BF)
        qkv[1] = rk
        qkv[2] = value
        wide = rk.astype(F32)
        left = left_head((HEAD, 128))
        for i in (0, 1):
            full = tn((wide * scale[2 + i]).astype(BF), value)
            packed = jnp.where(left, full[0:HEAD], full[HEAD:])
            for q in range(NY):
                msg_a[q, pl.ds(16 * i, 16)] = packed[16 * q : 16 * q + 16]

    def attend():
        qkv[0] = rotated(accb[0]).astype(BF)
        rk, value = qkv[1], qkv[2]

        def chunk(i, _):
            r = rows_of(i, 128)
            rq = qkv[0, r]
            left = left_head((128, 128))
            zero = jnp.zeros_like(rq)
            parts = []
            for h, own_q in enumerate((jnp.where(left, rq, zero), jnp.where(left, zero, rq))):
                probs = (nt(own_q, rk) * D[h, r]).astype(BF)
                parts.append(nn(probs, value))
            mix[r, pl.ds(0, 128)] = jnp.where(left, parts[0], parts[1])
            return 0

        lax.fori_loop(0, 4, chunk, 0, unroll=True)

    def inner_value():
        return (accb[1].astype(BF).astype(F32) * accb[2].astype(BF).astype(F32)).astype(BF).astype(F32)

    def halo_send():
        inner = inner_value()
        halo_s[0] = inner[0:8]
        halo_s[1] = inner[SPAN - 8 :]
        push(halo_s.at[1], halo_r.at[0], 7, hr.at[0], (lax.rem(s + 1, NZ * NY), t))
        push(halo_s.at[0], halo_r.at[1], 7, hr.at[1], (lax.rem(s + NZ * NY - 1, NZ * NY), t))

    def convolve():
        for i in (0, 1):
            took(halo_r.at[i], hr.at[i])
        inner = inner_value()
        row = lax.broadcasted_iota(jnp.int32, (SPAN, 128), 0)
        before = jnp.where(s == 0, 0.0, halo_r[0, 7:8, :])
        after = jnp.where(s == NZ * NY - 1, 0.0, halo_r[1, 0:1, :])
        prev = jnp.where(row == 0, before, pltpu.roll(inner, 1, axis=0))
        follow = jnp.where(row == SPAN - 1, after, pltpu.roll(inner, SPAN - 1, axis=0))
        conv = taps[0:1, :] * prev + taps[1:2, :] * inner + taps[2:3, :] * follow
        CR[:, pl.ds(0, 128)] = (acca[1].astype(BF).astype(F32) * conv).astype(BF)

    def spread_states():
        for dy in (1, 2, 3):
            yy = ring(y, dy, NY)
            push(msg_a.at[yy], got_a.at[y], 8, sar.at[dy - 1], at(dy=dy))
        got_a[y] = msg_a[y]

    def step_terms():
        return [
            (got_a[m, pl.ds(0, 16)], got_a[m, pl.ds(16, 16)], jnp.exp(got_a[m, pl.ds(32, 1)]), jnp.exp(got_a[m, pl.ds(33, 1)]))
            for m in range(NY)
        ]

    def spread_rows():
        for dy in (1, 2, 3):
            took(got_a.at[ring(y, -dy, NY)], sar.at[dy - 1])
        terms = step_terms()
        fwd, bwd = terms[0][0], terms[NY - 1][1]
        for m in range(1, NY):
            fwd = terms[m][2] * fwd + terms[m][0]
            back = terms[NY - 1 - m]
            bwd = back[3] * bwd + back[1]
        msg_b[0, pl.ds(0, 16)] = fwd
        msg_b[1, pl.ds(0, 16)] = bwd
        for i in (0, 1):
            total = got_a[0, pl.ds(32 + i, 1)]
            for m in range(1, NY):
                total = total + got_a[m, pl.ds(32 + i, 1)]
            msg_b[i, pl.ds(16, 8)] = jnp.broadcast_to(total, (8, 128))
        for d in (8, 7, 9, 6, 10, 5, 11, 4, 12, 3, 13, 2, 14, 1, 15):
            push(msg_b.at[(z + d) // NZ], got_b.at[d], 9, sbr.at[d], at(dz=d))

    def return_rows():
        for d in range(1, NZ):
            took(got_b.at[d], sbr.at[d])
        fwd = jnp.zeros((16, 128), F32)
        bwd = jnp.zeros((16, 128), F32)
        for d in range(NZ - 1, 0, -1):
            lower = jnp.exp(got_b[d, pl.ds(16, 1)]) * fwd + got_b[d, pl.ds(0, 16)]
            fwd = jnp.where(d <= z, lower, fwd)
            e = NZ - d
            higher = jnp.exp(got_b[e, pl.ds(16, 1)]) * bwd + got_b[e, pl.ds(0, 16)]
            bwd = jnp.where(d <= NZ - 1 - z, higher, bwd)
        terms = step_terms()
        for m in range(NY):
            msg_c[m, pl.ds(0, 16)] = fwd.astype(BF)
            fwd = terms[m][2] * fwd + terms[m][0]
            n = NY - 1 - m
            msg_c[n, pl.ds(16, 16)] = bwd.astype(BF)
            bwd = terms[n][3] * bwd + terms[n][1]
        for dy in (2, 1, 3):
            yy = ring(y, dy, NY)
            push(msg_c.at[yy], got_c.at[y], 10, scr.at[dy - 1], at(dy=dy))
        got_c[y] = msg_c[y]

    def finish():
        for dy in (1, 2, 3):
            took(got_c.at[ring(y, -dy, NY)], scr.at[dy - 1])
        left = left_head((HEAD, 128))
        into = []
        for i in (0, 1):
            packed = jnp.concatenate([got_c[q, pl.ds(16 * i, 16)] for q in range(NY)], axis=0)
            zero = jnp.zeros_like(packed)
            into.append(jnp.concatenate([jnp.where(left, packed, zero), jnp.where(left, zero, packed)], axis=0))
        both = jnp.concatenate(into, axis=1)
        same = (
            (lax.broadcasted_iota(jnp.int32, (128, 128), 0) < HEAD) == (lax.broadcasted_iota(jnp.int32, (128, 128), 1) < HEAD)
        ).astype(F32) * (1.0 / HEAD)
        same = same.astype(BF)

        def chunk(i, _):
            r = rows_of(i, 128)
            carried = nn(qkv[0, r], both)
            m = mix[r, pl.ds(0, 128)] + scale[0, r] * carried[:, :128] + scale[1, r] * carried[:, 128:]
            square = m * m
            high = square.astype(BF)
            inv = lax.rsqrt(nn(high, same) + nn((square - high.astype(F32)).astype(BF), same) + EPS)
            g = acca[0, r].astype(BF).astype(F32)
            silu = g / (1.0 + jnp.exp(-g))
            CR[r, pl.ds(128, 128)] = (silu * (m * inv * head_gain[...])).astype(BF)
            return 0

        lax.fori_loop(0, 4, chunk, 0)

    def out_rows(xo):
        rows = CR[rows_of(ring(x, xo, NX), 128)]
        for h in (0, 1):
            for n in (0, 1):
                res = nn(rows, WO[:, pl.ds(1024 * h + 512 * n, 512)]).astype(BF).reshape(2, 64, 512)
                part[xo, :, h, :, pl.ds(512 * n, 512)] = res
            push(part.at[xo, 1 - c, h], pair.at[xo, h], 11, dr.at[xo, h], at(dc=1))

    def summed(xo, half):
        took(pair.at[xo, half], dr.at[xo, half])
        return part[xo, c, half].astype(F32) + pair[xo, half].astype(F32)

    def far_out():
        for h in (0, 1):
            quads[2, h] = summed(2, h).astype(BF)
            push(quads.at[2, h], via.at[h], 12, vr.at[h], at(dx=SIDES[h]))

    def near_out():
        for xo, d in ((1, 0), (3, 1)):
            quads[xo, 1 - d] = summed(xo, 1 - d).astype(BF)
            push(quads.at[xo, 1 - d], fin.at[d, 1 - d], 13, fr.at[d, 1 - d], at(dx=SIDES[d]))

    def last_out():
        sums = [summed(xo, d) for xo, d in ((1, 0), (3, 1))]
        for xo, d in ((1, 0), (3, 1)):
            took(via.at[d], vr.at[d])
            quads[xo, d] = (sums[d] + via[d].astype(F32)).astype(BF)
            push(quads.at[xo, d], fin.at[d, d], 13, fr.at[d, d], at(dx=SIDES[d]))

    def own_out():
        for h in (0, 1):
            total = summed(0, h)
            for d in (1 - h, h):
                took(fin.at[d, h], fr.at[d, h])
                total = total + fin[d, h].astype(F32)
            done[:, pl.ds(1024 * h, 1024)] = total.astype(BF)
            pltpu.make_async_copy(done.at[:, pl.ds(1024 * h, 1024)], out.at[:, pl.ds(1024 * h, 1024)], outs.at[h]).start()

    def leave():
        all_left(WK.at[pl.ds(0, 15), 0], 0)
        all_left(WK.at[pl.ds(0, 12)], 1)
        all_left(WA.at[pl.ds(0, 15), 0], 2)
        all_left(WB.at[pl.ds(0, 15)], 3)
        all_left(WA.at[pl.ds(0, 12)], 4)
        all_left(WB.at[0, pl.ds(0, 3)], 5)
        all_left(X.at[pl.ds(0, 14)], 6)
        all_left(halo_s, 7)
        all_left(msg_a.at[pl.ds(0, 3)], 8)
        all_left(got_b.at[pl.ds(0, 15)], 9)
        all_left(msg_c.at[pl.ds(0, 3)], 10)
        all_left(pair, 11)
        all_left(via, 12)
        all_left(fin, 13)
        for h in (0, 1):
            cols = pl.ds(1024 * h, 1024)
            pltpu.make_async_copy(done.at[:, cols], out.at[:, cols], outs.at[h]).wait()

    own_here()
    greeted()
    send_kv(1)
    send_kv(2)
    yb_direct()
    send_zb(1, 0)
    y_kv(0)
    x_start()
    send_za(1)
    ya_direct(0)
    xpush(t, None, 6, at(dc=1))
    decay_sums()
    for k in range(1, 9):
        if k <= 4:
            recv_kv(2 * k)
            if k < 4:
                send_kv(2 * k + 1)
                send_kv(2 * k + 2)
            y_kv(2 * k)
            recv_kv(2 * k - 1)
            y_kv(2 * k - 1)
        if k == 1:
            for j in (1, 3, 2):
                yb_take(j)
                send_zb(1, j)
        recv_za(k)
        if k < 8:
            send_za(k + 1)
        ya_direct(k)
        if k == 2:
            x_onward()
        for j in (0, 1, 3, 2):
            recv_zb(k, j)
            if k < 8:
                send_zb(k + 1, j)
        ya_onward(k - 1)
        if k == 1:
            decay_matrix(0)
        if k == 2:
            decay_matrix(1)
            decay_scales()
            x_partner()
        if k == 3:
            angles()
            x_far()
        if k == 4:
            x_all()
            normalise()
        if k == 5:
            took(WK.at[pl.ds(0, 12)], kyr.at[0])
            project_kv()
            states()
            spread_states()
        if k == 6:
            project_b(1, 2, 3)
        if k == 7:
            spread_rows()
            project_b(4, 5)
        if k == 8:
            project_b(6, 7)
            took(WA.at[pl.ds(0, 11), 0], yahr.at[0])
    ya_onward(8)
    project_b(0, 8)
    halo_send()
    return_rows()
    attend()
    project_a(0, 1, 2, 3, 4, 5)
    for k in range(0, 6):
        turn_output(k)
    took(WA.at[pl.ds(0, 5), 0], yahr.at[1])
    project_a(6, 7, 8)
    for k in range(6, 9):
        turn_output(k)
    convolve()
    finish()
    for xo in (2, 1, 3):
        out_rows(xo)
    far_out()
    near_out()
    out_rows(0)
    last_out()
    own_out()
    leave()


def mixer(tok, gain, outer, inner, conv, query, key, value, gate, taps, decay, head_gain, conv_o, ret_o):
    dma = pltpu.SemaphoreType.DMA
    anywhere = pl.BlockSpec(memory_space=pl.ANY)
    return pl.pallas_call(
        mixer_kernel,
        out_shape=jax.ShapeDtypeStruct((64, 2048), BF),
        in_specs=[anywhere] * 14,
        out_specs=anywhere,
        scratch_shapes=[
            pltpu.VMEM((16, 128), F32),
            pltpu.VMEM((3, 128), F32),
            pltpu.VMEM((2, 2, SPAN), F32),
            pltpu.VMEM((1, 128), F32),
            pltpu.VMEM((16, SPAN, 128), BF),
            pltpu.VMEM((16, SPAN, 128), BF),
            pltpu.VMEM((NZ, NY, KROWS, 128), BF),
            pltpu.VMEM((NZ, NY, AROWS, 128), BF),
            pltpu.VMEM((NZ, NY, BROWS, 128), BF),
            pltpu.VMEM((256, 2048), BF),
            pltpu.VMEM((2, SPAN, 128), F32),
            pltpu.VMEM((3, SPAN, 128), F32),
            pltpu.VMEM((2, SPAN, 128), F32),
            pltpu.VMEM((2, SPAN, SPAN), F32),
            pltpu.VMEM((4, SPAN, 128), F32),
            pltpu.VMEM((2, SPAN, 128), F32),
            pltpu.VMEM((3, SPAN, 128), BF),
            pltpu.VMEM((SPAN, 512), F32),
            pltpu.VMEM((SPAN, 256), BF),
            pltpu.VMEM((2, 8, 128), F32),
            pltpu.VMEM((2, 8, 128), F32),
            pltpu.VMEM((NY, 40, 128), F32),
            pltpu.VMEM((NY, 40, 128), F32),
            pltpu.VMEM((2, 24, 128), F32),
            pltpu.VMEM((NZ, 24, 128), F32),
            pltpu.VMEM((NY, 32, 128), BF),
            pltpu.VMEM((NY, 32, 128), BF),
            pltpu.VMEM((NX, 2, 2, 64, 1024), BF),
            pltpu.VMEM((NX, 2, 64, 1024), BF),
            pltpu.VMEM((NX, 2, 64, 1024), BF),
            pltpu.VMEM((2, 64, 1024), BF),
            pltpu.VMEM((2, 2, 64, 1024), BF),
            pltpu.VMEM((64, 2048), BF),
            dma((15,)), dma((2, 8)), dma((1,)), dma((2, 8)), dma((2, 8, 4)), dma((2, 16)), dma((2,)), dma((3,)),
            dma((10,)), dma((2,)), dma((3,)), dma((16,)), dma((3,)), dma((4, 2)), dma((2,)), dma((2, 2)), dma((14,)),
            dma((2,)),
        ],
        compiler_params=pltpu.CompilerParams(
            collective_id=0, has_side_effects=True, vmem_limit_bytes=56 * 1024 * 1024
        ),
    )(
        tok, gain.reshape(16, 128), outer, inner, conv, query, key, value, gate, taps, decay,
        head_gain.reshape(1, 128), conv_o.T, ret_o.T,
    )


def solution(mesh):
    return jax.shard_map(
        mixer,
        mesh=mesh,
        in_specs=(
            P("sp", "tp"),
            P(),
            P("sp", "tp"),
            P("sp", "tp"),
            P("sp", "tp"),
            P("sp", "tp"),
            P("sp", "tp"),
            P("sp", "tp"),
            P("sp", "tp"),
            P(None, "tp"),
            P(None, "tp", "sp"),
            P("tp"),
            P("tp", "sp"),
            P("tp", "sp"),
        ),
        out_specs=P(("sp", "tp"), None),
        check_vma=False,
    )
```
